256 devices in a mesh: sp: 16 (over y, x), tp: 16 (over z, core).
Axes of the slice: x: 4, y: 4, z: 8, core: 2. Of those that a mesh axis runs over, the one named last changes fastest.
Arguments:
- layer_in: bfloat16 [5120, 2048], P('sp', 'tp'), may hold values from -6 to 6
- out_cot: bfloat16 [5120, 2048], P('sp', 'tp'), may hold values from -6 to 6
- route_ids: int32 [5120, 2], P('sp'), may hold values from 0 to 15, all different within a row; in each aligned block of 320 rows (0 to 319, 320 to 639, ...) at most 80 rows name the same one
- route_probs: float32 [5120, 2], P('sp'), may hold values from 0.2 to 1
- group_prob: float32 [5120], P('sp'), may hold values from 0.3 to 1
- gate_weight: bfloat16 [16, 2048, 2048], P('sp', 'tp'), may hold values from -0.125 to 0.125
- up_weight: bfloat16 [16, 2048, 2048], P('sp', 'tp'), may hold values from -0.125 to 0.125
- down_weight: bfloat16 [16, 2048, 2048], P('sp', 'tp'), may hold values from -0.125 to 0.125
- out_weight: bfloat16 [2048, 2048], P(None, 'tp'), may hold values from -0.125 to 0.125
- query: bfloat16 [5120, 1024], P('sp', 'tp'), may hold values from -6 to 6
- key_in: bfloat16 [5120, 1024], P('sp', 'tp'), may hold values from -0.75 to 0.75
- value: bfloat16 [5120, 2048], P('sp', 'tp'), may hold values from -6 to 6
- decay_logit: bfloat16 [5120, 1024], P('sp', 'tp'), may hold values from -2.5 to 8.5, as said below
Outputs:
- gate_grad: float32 [16, 2048, 2048], P('sp', 'tp')
- up_grad: float32 [16, 2048, 2048], P('sp', 'tp')
- down_grad: float32 [16, 2048, 2048], P('sp', 'tp')
- proj_grad: float32 [2048, 2048], P('sp', 'tp')
- query_grad: float32 [5120, 1024], P('sp', 'tp')
- key_grad: float32 [5120, 1024], P('sp', 'tp')
- value_grad: float32 [5120, 2048], P('sp', 'tp')
- logit_grad: float32 [5120, 1024], P('sp', 'tp')
The draws below stay inside these ranges and needn't reach their ends.
Inputs may be any that keep to these rules, and one draw needn't show every extreme that they name: `route_ids`: each row names two different experts of 0 to 15; every expert is named by some row; within each aligned block of 320 rows (the rows of one device) no expert is named more than 80 times, and in some block one expert is named exactly 80 times. `decay_logit`: values lie between -2.5 and 8.5; even heads have pre-activations near 5, odd heads near 1.
All inputs are finite; a program needn't handle non-finite values.
Results may differ from the reference program's by a relative error of at most 0.019.
Values may be sent and summed in bfloat16 or wider, within the bound.
No kernel may reach another device: no remote copies, remote signals or barrier semaphores. Data moves between devices by JAX's collectives and lax.ppermute only.
A program may use at most 128 MiB of HBM per device.

```python
import math
import jax
import jax.numpy as jnp
import numpy as np
from jax import lax

D = 2048
FFE = 2048
HEADS = 16
DK = 64
DV = 128
BLOCK = 64
TOK_DEV = 320
TOKENS = 5120
EXPERTS = 16
CAP = 80
N_SP = 16
N_TP = 16


def draw_decay_logit(key, part):
    shift_key, noise_key = jax.random.split(key, 2)
    channel_head = jnp.arange(HEADS * DK) // DK
    base_level = jnp.where(channel_head % 2 == 0, 5.0, 1.0)
    span_shift = jax.random.uniform(shift_key, (TOKENS // TOK_DEV, HEADS), minval=-0.8, maxval=0.8)
    row_span = jnp.arange(TOKENS) // TOK_DEV
    slow_part = span_shift[row_span][:, channel_head]
    noise_part = jnp.clip(0.6 * jax.random.normal(noise_key, (TOKENS, HEADS * DK)), -2.4, 2.4)
    return (base_level[None, :] + slow_part + noise_part).astype(jnp.float32).astype(jnp.bfloat16)


def raised(entries, rng, source, target, blocks, factor):
    owner, partner = [(jnp.arange(entries.shape[axis_at]) // (entries.shape[axis_at] // blocks)).reshape([-1 if axis == axis_at else 1 for axis in range(entries.ndim)]) for axis_at in (source, target)]
    chosen = jax.random.permutation(rng, blocks)[partner]
    strong = (owner == chosen) | (owner == (partner + blocks // 2) % blocks)
    return jnp.where(strong, factor * entries, entries)


def block_scale(rng, shape, cuts, least, largest):
    gain = 1.0
    for position, blocks in cuts:
        draws = jax.random.uniform(jax.random.fold_in(jax.random.fold_in(rng, 6), position), (blocks,), jnp.float32, least / len(cuts), largest / len(cuts))
        gain = gain * jnp.repeat(jnp.exp(draws), shape[position] // blocks).reshape((-1,) + (1,) * (len(shape) - 1 - position))
    return gain


def shared_out(stream_key, own, number, rows, count, top, most, slope):
    sequence = jax.random.permutation(stream_key, count)
    crowded, ordinary = load_shares(count, rows * top, most, slope, True), load_shares(count, rows * top, most, slope, False)
    places = jnp.arange(count)

    def named(sizes, turn):
        used = int((sizes > 0).sum())
        fixed = max(1, used // 4)
        passed = fixed + (places - fixed + turn * (used - fixed)) % max(1, count - fixed)
        return jnp.zeros((count,), jnp.int32).at[sequence[jnp.where(places < fixed, places, passed)]].set(jnp.asarray(sizes, jnp.int32))

    sizes = jnp.where(number % 4 == 0, named(crowded, number // 4), named(ordinary, number - number // 4 - 1))
    mixed = jax.random.permutation(jax.random.fold_in(own, 3), count)
    giver, receiver = mixed[0:count // 2 * 2:2], mixed[1:count // 2 * 2:2]
    room = jnp.minimum(sizes[giver] - 1, most - sizes[receiver]) // 2
    room = jnp.where((giver == sequence[0]) | (receiver == sequence[0]) | (sizes[receiver] == 0), 0, jnp.maximum(room, 0))
    passed = jax.random.randint(jax.random.fold_in(own, 4), (count // 2,), 0, 1 << 20) % (room + 1)
    sizes = sizes.at[giver].add(-passed).at[receiver].add(passed)
    items = jnp.searchsorted(jnp.cumsum(sizes), jnp.arange(rows * top), side="right").astype(jnp.int32)
    grid = items.reshape(top, rows).T
    grid = grid[jax.random.permutation(jax.random.fold_in(own, 1), rows)]
    turn = jax.random.randint(jax.random.fold_in(own, 2), (rows, 1), 0, top)
    return jnp.take_along_axis(grid, (jnp.arange(top)[None, :] + turn) % top, axis=1)


def load_shares(amount, total, reach, skew, full):
    weights = [(1 << 20) // math.isqrt(rank ** skew) + 1 for rank in range(1, amount + 1)]
    largest = reach if full else min(reach, max(-(-total // amount), total * weights[0] // sum(weights)))
    least = 1 if total - largest >= amount - 1 else 0
    given, surplus = [largest] + [least] * (amount - 1), total - largest - least * (amount - 1)
    while surplus > 0:
        candidates = [i for i in range(1, amount) if given[i] < largest] or [i for i in range(1, amount) if given[i] < reach]
        whole, budget = sum([weights[i] for i in candidates]), surplus
        for i in candidates:
            addition = min(reach - given[i], max(1, budget * weights[i] // whole), surplus)
            given[i] = given[i] + addition
            surplus = surplus - addition
    return np.array(given)


def normal_values(rng, dims, deviation, limit, cuts=(), held_as=jnp.bfloat16):
    level = block_scale(rng, dims, cuts, -0.22, 0.18) if cuts else 1.0
    entries = jax.random.normal(rng, dims, jnp.float32) * deviation * level
    return jnp.minimum(jnp.maximum(entries, -limit), limit).astype(held_as)


def noise_with(key, shape, scale, most, cuts, heavy, held_as=jnp.bfloat16):
    drawn = scale * jax.random.normal(key, shape, jnp.float32)
    if cuts:
        drawn = drawn * block_scale(key, shape, cuts, -0.22, 0.18)
    return jnp.clip(raised(drawn, jax.random.fold_in(key, 3), *heavy), -most, most).astype(held_as)


def setup_inputs(seed: int = 0) -> dict:
    streams_of = jax.random.split(jax.random.key(seed), 14)
    layer_in = normal_values(streams_of[0], (TOKENS, D), 1.0, 6.0, ((0, 16), (1, 16)))
    out_cot = noise_with(streams_of[1], (TOKENS, D), 1.0, 6.0, ((0, 16), (1, 16)), (0, 1, 16, 2.0))
    route_ids_keys = jax.random.split(jax.random.fold_in(streams_of[2], 1), TOKENS // TOK_DEV)
    route_ids_turns = jax.random.permutation(jax.random.fold_in(streams_of[2], 3), TOKENS // TOK_DEV)
    route_ids = jax.vmap(lambda own, number: shared_out(jax.random.fold_in(streams_of[2], 2), own, number, TOK_DEV, EXPERTS, 2, CAP, 1))(route_ids_keys, route_ids_turns).reshape((TOKENS, 2))
    route_probs = jnp.clip(0.2 + 0.8 * jax.random.uniform(streams_of[3], (TOKENS, 2), jnp.float32) ** block_scale(streams_of[3], (TOKENS, 2), ((0, 16),), -0.2, 0.2), 0.2, 1.0)
    group_prob = jnp.clip(0.3 + 0.7 * jax.random.uniform(streams_of[4], (TOKENS,), jnp.float32) ** block_scale(streams_of[4], (TOKENS,), ((0, 16),), -0.2, 0.2), 0.3, 1.0)
    gate_weight = normal_values(streams_of[5], (EXPERTS, FFE, D), D ** -0.5, 0.125, ((0, 16), (1, 16)))
    up_weight = normal_values(streams_of[6], (EXPERTS, FFE, D), D ** -0.5, 0.125, ((0, 16), (1, 16)))
    down_weight = normal_values(streams_of[7], (EXPERTS, FFE, D), FFE ** -0.5, 0.125, ((0, 16), (1, 16)))
    out_weight = normal_values(streams_of[8], (D, HEADS * DV), (HEADS * DV) ** -0.5, 0.125, ((1, 16),))
    query = normal_values(streams_of[9], (TOKENS, HEADS * DK), 1.0, 6.0, ((0, 16), (1, 16)))
    key_in = normal_values(streams_of[10], (TOKENS, HEADS * DK), 0.125, 0.75, ((0, 16), (1, 16)))
    value = normal_values(streams_of[11], (TOKENS, HEADS * DV), 1.0, 6.0, ((0, 16), (1, 16)))
    decay_logit = draw_decay_logit(jax.random.fold_in(streams_of[13], 71), 0)
    return dict(layer_in=layer_in, out_cot=out_cot, route_ids=route_ids, route_probs=route_probs, group_prob=group_prob, gate_weight=gate_weight, up_weight=up_weight, down_weight=down_weight, out_weight=out_weight, query=query, key_in=key_in, value=value, decay_logit=decay_logit)


decay_temp = 16.0
highest = lax.Precision.HIGHEST

def mixer_forward(scaled_query, keys_all, values_all, log_decay):
    length_all, head_count, key_dim = scaled_query.shape
    val_dim = values_all.shape[-1]
    blocks = length_all // BLOCK

    def split_blocks(tensor):
        return tensor.reshape(blocks, BLOCK, head_count, tensor.shape[-1]).transpose(2, 0, 1, 3)
    query_blk = split_blocks(scaled_query)
    key_blk = split_blocks(keys_all)
    value_blk = split_blocks(values_all)
    cumulative = jnp.cumsum(split_blocks(log_decay), axis=2)
    span_log = cumulative[:, :, -1:, :]
    query_decayed = query_blk * jnp.exp(cumulative)
    key_back = key_blk * jnp.exp(-cumulative)
    key_to_end = key_blk * jnp.exp(span_log - cumulative)
    causal = jnp.tril(jnp.ones((BLOCK, BLOCK), dtype=bool))
    scores = jnp.where(causal, jnp.einsum('hncd,hnsd->hncs', query_decayed, key_back, precision=highest), 0.0)
    within = jnp.einsum('hncs,hnsv->hncv', scores, value_blk, precision=highest)
    update = jnp.einsum('hncd,hncv->hndv', key_to_end, value_blk, precision=highest)
    block_decay = jnp.exp(span_log[:, :, 0, :])

    def advance(carry_state, inputs):
        decay_now, update_now = inputs
        return (carry_state * decay_now[..., None] + update_now, carry_state)
    start_state = jnp.zeros((head_count, key_dim, val_dim), jnp.float32)
    _, entering = lax.scan(advance, start_state, (jnp.moveaxis(block_decay, 1, 0), jnp.moveaxis(update, 1, 0)))
    entering = jnp.moveaxis(entering, 0, 1)
    carried = jnp.einsum('hncd,hndv->hncv', query_decayed, entering, precision=highest)
    return (within + carried).transpose(1, 2, 0, 3).reshape(length_all, head_count * val_dim)

def reference(layer_in, out_cot, route_ids, route_probs, group_prob, gate_weight, up_weight, down_weight, out_weight, query, key_in, value, decay_logit):
    length_all = layer_in.shape[0]
    width = layer_in.shape[1]
    route_weight = group_prob[:, None] * route_probs / lax.optimization_barrier(jnp.sum(route_probs, axis=1, keepdims=True))
    scaled_cot = (route_weight[:, :, None] * out_cot.astype(jnp.float32)[:, None, :]).astype(jnp.bfloat16)
    flat_ids = route_ids.reshape(-1)
    flat_cot = scaled_cot.reshape(-1, width)
    rows_max = N_SP * CAP
    hidden_dev = FFE // N_TP

    def one_expert(expert):
        order_rows = jnp.argsort((flat_ids != expert).astype(jnp.int32), stable=True)[:rows_max]
        valid_rows = flat_ids[order_rows] == expert
        token_rows = (order_rows // 2).astype(jnp.int32)
        inputs_x = layer_in[token_rows]
        cot_rows = jnp.where(valid_rows[:, None], flat_cot[order_rows], jnp.zeros((), jnp.bfloat16))
        gate_mat = gate_weight[expert]
        up_mat = up_weight[expert]
        down_mat = down_weight[expert]
        gate_pre = jnp.dot(inputs_x, gate_mat.T, preferred_element_type=jnp.float32)
        up_pre = jnp.dot(inputs_x, up_mat.T, preferred_element_type=jnp.float32)
        sigmoid_gate = jax.nn.sigmoid(gate_pre)
        active = gate_pre * sigmoid_gate
        hidden = (active * up_pre).astype(jnp.bfloat16)
        hidden_cot = jnp.dot(cot_rows, down_mat.T, preferred_element_type=jnp.float32)
        up_cot = (hidden_cot * active).astype(jnp.bfloat16)
        gate_cot = (hidden_cot * up_pre * sigmoid_gate * (1.0 + gate_pre * (1.0 - sigmoid_gate))).astype(jnp.bfloat16)
        down_g = jnp.dot(hidden.T, cot_rows, preferred_element_type=jnp.float32)
        gate_g = jnp.dot(gate_cot.T, inputs_x, preferred_element_type=jnp.float32)
        up_g = jnp.dot(up_cot.T, inputs_x, preferred_element_type=jnp.float32)
        gate_groups = gate_cot.astype(jnp.float32).reshape(rows_max, N_TP, hidden_dev)
        up_groups = up_cot.astype(jnp.float32).reshape(rows_max, N_TP, hidden_dev)
        gate_split = gate_mat.astype(jnp.float32).reshape(N_TP, hidden_dev, width)
        up_split = up_mat.astype(jnp.float32).reshape(N_TP, hidden_dev, width)
        partial_sum = jnp.einsum('rjf,jfd->rjd', gate_groups, gate_split, precision=highest)
        partial_sum = partial_sum + jnp.einsum('rjf,jfd->rjd', up_groups, up_split, precision=highest)
        rounded = lax.optimization_barrier(partial_sum.astype(jnp.bfloat16)).astype(jnp.float32)
        input_grad = lax.optimization_barrier(jnp.sum(rounded, axis=1))
        return (gate_g, up_g, down_g, input_grad, token_rows)
    gate_grad, up_grad, down_grad, input_grads, token_index = lax.map(one_expert, jnp.arange(EXPERTS, dtype=jnp.int32))
    routed_sum = jax.ops.segment_sum(input_grads.reshape(-1, width), token_index.reshape(-1), num_segments=length_all)
    mixed_cot = (out_cot.astype(jnp.float32) + routed_sum).astype(jnp.bfloat16)
    mixer_cot = jnp.dot(mixed_cot, out_weight, preferred_element_type=jnp.float32)

    def forward(query_f, key_f, value_f, logit_f):
        scaled = query_f.reshape(length_all, HEADS, DK) * DK ** (-0.5)
        log_decay = (jax.nn.log_sigmoid(logit_f) / decay_temp).reshape(length_all, HEADS, DK)
        return mixer_forward(scaled, key_f.reshape(length_all, HEADS, DK), value_f.reshape(length_all, HEADS, DV), log_decay)
    mixer_f32, pullback = jax.vjp(forward, query.astype(jnp.float32), key_in.astype(jnp.float32), value.astype(jnp.float32), decay_logit.astype(jnp.float32))
    query_grad, key_grad, value_grad, logit_grad = pullback(mixer_cot)
    mixer_out = mixer_f32.astype(jnp.bfloat16)
    proj_grad = jnp.dot(mixed_cot.T, mixer_out, preferred_element_type=jnp.float32)
    return (gate_grad, up_grad, down_grad, proj_grad, query_grad, key_grad, value_grad, logit_grad)
```

```python
import jax
import jax.numpy as jnp
from jax import lax
from jax.sharding import PartitionSpec as P

DK = 64
DV = 128
BLOCK = 64


decay_temp = 16.0
highest = lax.Precision.HIGHEST
f32 = jnp.float32
bf16 = jnp.bfloat16


def dot(a, b, dims):
    return lax.dot_general(a, b, (dims, ((), ())), preferred_element_type=f32)


def shifted(x, hops):
    size = lax.axis_size("tp")
    return lax.ppermute(x, "tp", [(i, (i + 2 * hops) % size) for i in range(size)])


def swapped(x):
    return lax.ppermute(x, "tp", [(i, i ^ 1) for i in range(lax.axis_size("tp"))])


def ring_gather(x, right_steps, left_steps):
    found = {0: x}
    right = left = x
    for s in range(1, max(right_steps, left_steps) + 1):
        if s <= right_steps:
            right = shifted(right, 1)
            found[-s] = right
        if s <= left_steps:
            left = shifted(left, -1)
            found[s] = left
    return found


def columns(mat, block, width):
    return lax.dynamic_slice_in_dim(mat, block * width, width, axis=1)


def bmm(spec, a, b):
    return jnp.einsum(spec, a, b, precision=highest)


def local(
    layer_in,
    out_cot,
    route_ids,
    route_probs,
    group_prob,
    gate_weight,
    up_weight,
    down_weight,
    out_weight,
    query,
    key_in,
    value,
    decay_logit,
):
    tok_rows, local_cols = layer_in.shape
    experts_all = lax.axis_size("sp")
    capacity = 4 * tok_rows // experts_all
    chips = lax.axis_size("tp") // 2
    far = chips // 2
    place = lax.axis_index("tp")
    chip, core = place // 2, place % 2
    mine = lax.axis_index("sp")

    def block_at(distance, other=0):
        return 2 * ((chip + distance) % chips) + (core ^ other)

    blocks = tok_rows // BLOCK
    split = lambda a: a.astype(f32).reshape(blocks, BLOCK, -1)
    scaled_query = split(query) * DK ** (-0.5)
    key_blk, value_blk, logit_blk = split(key_in), split(value), split(decay_logit)
    log_decay = jax.nn.log_sigmoid(logit_blk) / decay_temp
    causal = jnp.tril(jnp.ones((BLOCK, BLOCK), dtype=bool))
    cumulative = jnp.einsum(
        "cs,nsd->ncd", causal.astype(f32), log_decay, precision=highest
    )
    span_log = cumulative[:, -1:, :]
    to_end = jnp.exp(span_log - cumulative)
    key_to_end = key_blk * to_end
    block_decay = jnp.exp(span_log[:, 0, :])
    block_update = bmm("ncd,ncv->ndv", key_to_end, value_blk)
    before, state, so_far = [], jnp.zeros((DK, DV), f32), jnp.zeros((DK,), f32)
    for n in range(blocks):
        before.append((so_far, state))
        state = state * block_decay[n][:, None] + block_update[n]
        so_far = so_far + span_log[n, 0]
    total_log = so_far

    ids = route_ids.T
    probs = route_probs.T
    route_weight = group_prob[None] * probs / jnp.sum(probs, axis=0, keepdims=True)
    numbers = jnp.arange(experts_all, dtype=jnp.int32)[:, None]
    first, second = (ids[j][None] == numbers for j in (0, 1))
    named = first | second
    steps = jnp.arange(tok_rows)
    earlier = (steps[:, None] < steps[None, :]).astype(bf16)
    position = dot(named.astype(bf16), earlier, ((1,), (0,))).astype(jnp.int32)
    weight_of = jnp.where(first, route_weight[0][None], route_weight[1][None])
    chosen = named[:, None, :] & (
        position[:, None, :] == jnp.arange(capacity, dtype=jnp.int32)[None, :, None]
    )
    select = chosen.astype(bf16).reshape(experts_all * capacity, tok_rows)
    row_weight = jnp.sum(jnp.where(chosen, weight_of[:, None, :], 0.0), axis=2)
    send_x = dot(select, layer_in, ((1,), (0,))).astype(bf16)
    send_cot = (
        dot(select, out_cot, ((1,), (0,))) * row_weight.reshape(-1, 1)
    ).astype(bf16)
    send_x = send_x.reshape(experts_all, capacity, local_cols)
    send_cot = send_cot.reshape(experts_all, capacity, local_cols)
    log_line = jnp.pad(total_log, (0, DV - DK))[None]
    leaving = jnp.pad(jnp.concatenate([state, log_line]), ((0, capacity - DK - 1), (0, 0)))
    leaving = jnp.broadcast_to(leaving.astype(bf16)[None], (experts_all, capacity, DV))
    received = lax.all_to_all(
        jnp.concatenate([send_x, send_cot, leaving], axis=1), "sp", 0, 0, tiled=True
    )
    rows = experts_all * capacity
    x_own = received[:, :capacity].reshape(rows, local_cols)
    cot_own = received[:, capacity : 2 * capacity].reshape(rows, local_cols)
    span_states = received[:, 2 * capacity : 2 * capacity + DK].astype(f32)
    span_logs = received[:, 2 * capacity + DK, :DK].astype(f32)

    gate_mat, up_mat, down_mat = (gate_weight[0], up_weight[0], down_weight[0])
    gate_up = jnp.concatenate([gate_mat, up_mat])
    hidden_here = gate_mat.shape[0]
    x_chunks = ring_gather(x_own, far, far - 1)
    cot_chunks = ring_gather(cot_own, far - 1, far)
    x_chunks[far] = x_chunks.pop(-far)
    pre = jnp.zeros((rows, 2 * hidden_here), f32)
    hidden_cot = jnp.zeros((rows, hidden_here), f32)
    order = [0]
    for s in range(1, far):
        order += [-s, s]
    order.append(far)
    x_all, cot_all = {}, {}
    for d in order:
        x_all[d] = (x_chunks[d], swapped(x_chunks[d]))
        cot_all[d] = (cot_chunks[d], swapped(cot_chunks[d]))
        for other in (0, 1):
            at = block_at(d, other)
            pre = pre + dot(x_all[d][other], columns(gate_up, at, local_cols), ((1,), (1,)))
            hidden_cot = hidden_cot + dot(
                cot_all[d][other], columns(down_mat, at, local_cols), ((1,), (1,))
            )

    gate_pre, up_pre = pre[:, :hidden_here], pre[:, hidden_here:]
    sigmoid_gate = jax.nn.sigmoid(gate_pre)
    active = gate_pre * sigmoid_gate
    hidden = (active * up_pre).astype(bf16)
    up_cot = (hidden_cot * active).astype(bf16)
    gate_cot = (
        hidden_cot * up_pre * sigmoid_gate * (1.0 + gate_pre * (1.0 - sigmoid_gate))
    ).astype(bf16)
    both_cot = jnp.concatenate([gate_cot, up_cot], axis=1)

    half = rows // 2
    halves = (slice(0, half), slice(half, rows))
    from_other = {}
    for d in (far, far - 1, 1 - far, *[e for s in range(far - 2, 0, -1) for e in (s, -s)], 0):
        part = dot(both_cot, columns(gate_up, block_at(d, 1), local_cols), ((1,), (0,)))
        from_other[d] = swapped(part.astype(bf16))

    def part_for(d, h):
        own = dot(both_cot[halves[h]], columns(gate_up, block_at(d), local_cols), ((1,), (0,)))
        return own + from_other[d][halves[h]].astype(f32)

    arrived = {}
    moving = {}
    for s in range(far, 0, -1):
        for h in (0, 1):
            for way in (1, -1):
                longest = far if (h == 0) == (way == 1) else far - 1
                if s > longest:
                    continue
                d = far if s == far else way * s
                part = part_for(d, h)
                if (h, way) in moving:
                    part = part + moving[h, way].astype(f32)
                moving[h, way] = shifted(part.astype(bf16), way)
    back = jnp.concatenate(
        [
            (part_for(0, h) + moving[h, 1].astype(f32) + moving[h, -1].astype(f32)).astype(bf16)
            for h in (0, 1)
        ]
    )
    returned = lax.all_to_all(
        back.reshape(experts_all, capacity, local_cols), "sp", 0, 0, tiled=True
    ).reshape(rows, local_cols)

    gate_up_g = jnp.zeros((2 * hidden_here, gate_mat.shape[1]), f32)
    down_g = jnp.zeros(down_mat.shape, f32)
    for d in order:
        for other in (0, 1):
            at = block_at(d, other) * local_cols
            gate_up_g = lax.dynamic_update_slice_in_dim(
                gate_up_g, dot(both_cot, x_all[d][other], ((0,), (0,))), at, axis=1
            )
            down_g = lax.dynamic_update_slice_in_dim(
                down_g, dot(hidden, cot_all[d][other], ((0,), (0,))), at, axis=1
            )
    gate_g, up_g = gate_up_g[:hidden_here], gate_up_g[hidden_here:]

    spans = jnp.arange(experts_all)
    between = (spans[None, :] > spans[:, None]) & (spans[None, :] < mine)
    weights = jnp.exp(jnp.dot(between.astype(f32), span_logs, precision=highest))
    weights = jnp.where((spans < mine)[:, None], weights, 0.0)
    entry_state = jnp.sum(weights[:, :, None] * span_states, axis=0)
    beyond = (spans[None, :] < spans[:, None]) & (spans[None, :] > mine)
    back_weights = jnp.exp(jnp.dot(beyond.astype(f32), span_logs, precision=highest))
    back_weights = jnp.where((spans > mine)[:, None], back_weights, 0.0)
    growth = jnp.exp(cumulative)
    shrink = jnp.exp(-cumulative)
    query_decayed = scaled_query * growth
    key_back = key_blk * shrink
    scores = jnp.where(causal, bmm("ncd,nsd->ncs", query_decayed, key_back), 0.0)
    block_state = jnp.stack(
        [jnp.exp(so)[:, None] * entry_state + st for so, st in before]
    )
    span_end = jnp.exp(total_log)[:, None] * entry_state + state
    outputs = bmm("ncs,nsv->ncv", scores, value_blk) + bmm(
        "ncd,ndv->ncv", query_decayed, block_state
    )
    mixer_out = outputs.reshape(tok_rows, DV).astype(bf16)

    routed_sum = dot(select, returned, ((0,), (0,)))
    mixed_own = (out_cot.astype(f32) + routed_sum).astype(bf16)
    mixer_cot = jnp.zeros((tok_rows, DV), f32)
    proj = jnp.zeros((2 * chips, local_cols, DV), bf16)
    for d in order:
        chunk = mixed_own if d == 0 else shifted(mixed_own, -d)
        for other in (0, 1):
            piece = swapped(chunk) if other else chunk
            at = block_at(d, other)
            mixer_cot = mixer_cot + dot(
                piece,
                lax.dynamic_slice_in_dim(out_weight, at * local_cols, local_cols, axis=0),
                ((1,), (0,)),
            )
            proj = lax.dynamic_update_slice_in_dim(
                proj, dot(piece, mixer_out, ((0,), (0,))).astype(bf16)[None], at, axis=0
            )
    proj_grad = jnp.sum(lax.all_to_all(proj, "sp", 0, 0, tiled=True).astype(f32), axis=0)

    cot_blk = mixer_cot.reshape(blocks, BLOCK, DV)
    block_future = bmm("ncd,ncv->ndv", query_decayed, cot_blk)
    after, back_state, back_log = [None] * blocks, jnp.zeros((DK, DV), f32), jnp.zeros((DK,), f32)
    for n in range(blocks - 1, -1, -1):
        after[n] = (back_log, back_state)
        back_state = back_state * block_decay[n][:, None] + block_future[n]
        back_log = back_log + span_log[n, 0]
    back_states = lax.all_to_all(
        jnp.broadcast_to(back_state.astype(bf16)[None], (experts_all, DK, DV)), "sp", 0, 0, tiled=True
    ).astype(f32)
    future_state = jnp.sum(back_weights[:, :, None] * back_states, axis=0)
    block_future_state = jnp.stack(
        [jnp.exp(lo)[:, None] * future_state + st for lo, st in after]
    )
    cot_values = jnp.where(causal, bmm("ncv,nsv->ncs", cot_blk, value_blk), 0.0)
    query_scaled_grad = growth * (
        bmm("ncv,ndv->ncd", cot_blk, block_state) + bmm("ncs,nsd->ncd", cot_values, key_back)
    )
    key_grad = shrink * bmm("ncs,ncd->nsd", cot_values, query_decayed) + to_end * bmm(
        "nsv,ndv->nsd", value_blk, block_future_state
    )
    value_grad = bmm("ncs,ncv->nsv", scores, cot_blk) + bmm(
        "nsd,ndv->nsv", key_to_end, block_future_state
    )
    terms = scaled_query * query_scaled_grad - key_blk * key_grad
    within_tail = jnp.einsum("cs,nsd->ncd", causal.T.astype(f32), terms, precision=highest)
    later_tail, tails = jnp.sum(future_state * span_end, axis=1), [None] * blocks
    for n in range(blocks - 1, -1, -1):
        tails[n] = within_tail[n] + later_tail[None]
        later_tail = later_tail + within_tail[n, 0]
    log_grad = jnp.stack(tails)
    logit_grad = log_grad * jax.nn.sigmoid(-logit_blk) / decay_temp
    flat = lambda a: a.reshape(tok_rows, -1)
    return (
        gate_g[None],
        up_g[None],
        down_g[None],
        proj_grad,
        flat(query_scaled_grad * DK ** (-0.5)),
        flat(key_grad),
        flat(value_grad),
        flat(logit_grad),
    )


def solution(mesh):
    in_specs = (
        P("sp", "tp"),
        P("sp", "tp"),
        P("sp", None),
        P("sp", None),
        P("sp"),
        P("sp", "tp", None),
        P("sp", "tp", None),
        P("sp", "tp", None),
        P(None, "tp"),
        P("sp", "tp"),
        P("sp", "tp"),
        P("sp", "tp"),
        P("sp", "tp"),
    )
    out_specs = (
        P("sp", "tp", None),
        P("sp", "tp", None),
        P("sp", "tp", None),
        P("sp", "tp"),
        P("sp", "tp"),
        P("sp", "tp"),
        P("sp", "tp"),
        P("sp", "tp"),
    )
    return jax.shard_map(local, mesh=mesh, in_specs=in_specs, out_specs=out_specs, check_vma=False)
```

```python
import jax
import jax.numpy as jnp
from jax import lax
from jax.sharding import PartitionSpec as P


DK = 64
DV = 128
BLOCK = 64


decay_temp = 16.0
highest = lax.Precision.HIGHEST
f32 = jnp.float32
bf16 = jnp.bfloat16


def dot(a, b, dims):
    return lax.dot_general(a, b, (dims, ((), ())), preferred_element_type=f32)


def onward(x, hops):
    size = lax.axis_size("tp")
    return lax.ppermute(
        x, "tp", [(i, (i + (2 * hops if i % 2 == 0 else -2 * hops)) % size) for i in range(size)]
    )


def swapped(x):
    return lax.ppermute(x, "tp", [(i, i ^ 1) for i in range(lax.axis_size("tp"))])


def columns(mat, block, width):
    return lax.dynamic_slice_in_dim(mat, block * width, width, axis=1)


def bmm(spec, a, b):
    return jnp.einsum(spec, a, b, precision=highest)


def local(
    layer_in,
    out_cot,
    route_ids,
    route_probs,
    group_prob,
    gate_weight,
    up_weight,
    down_weight,
    out_weight,
    query,
    key_in,
    value,
    decay_logit,
):
    tok_rows, local_cols = layer_in.shape
    experts_all = lax.axis_size("sp")
    capacity = 4 * tok_rows // experts_all
    chips = lax.axis_size("tp") // 2
    far = chips // 2
    place = lax.axis_index("tp")
    chip, core = place // 2, place % 2
    mine = lax.axis_index("sp")

    way = 1 - 2 * core

    def chip_at(distance):
        return (chip + distance) % chips

    def in_order(own, other):
        low = core == 0
        return jnp.concatenate([jnp.where(low, own, other), jnp.where(low, other, own)], axis=1)

    def after(x, y):
        return lax.optimization_barrier((x, y))[0]

    blocks = tok_rows // BLOCK
    split = lambda a: a.astype(f32).reshape(blocks, BLOCK, -1)
    scaled_query = split(query) * DK ** (-0.5)
    key_blk, value_blk, logit_blk = split(key_in), split(value), split(decay_logit)
    log_decay = jax.nn.log_sigmoid(logit_blk) / decay_temp
    causal = jnp.tril(jnp.ones((BLOCK, BLOCK), dtype=bool))
    cumulative = jnp.einsum(
        "cs,nsd->ncd", causal.astype(f32), log_decay, precision=highest
    )
    span_log = cumulative[:, -1:, :]
    to_end = jnp.exp(span_log - cumulative)
    key_to_end = key_blk * to_end
    block_decay = jnp.exp(span_log[:, 0, :])
    block_update = bmm("ncd,ncv->ndv", key_to_end, value_blk)
    before, state, so_far = [], jnp.zeros((DK, DV), f32), jnp.zeros((DK,), f32)
    for n in range(blocks):
        before.append((so_far, state))
        state = state * block_decay[n][:, None] + block_update[n]
        so_far = so_far + span_log[n, 0]
    total_log = so_far

    ids = route_ids.T
    probs = route_probs.T
    route_weight = group_prob[None] * probs / jnp.sum(probs, axis=0, keepdims=True)
    numbers = jnp.arange(experts_all, dtype=jnp.int32)[:, None]
    first, second = (ids[j][None] == numbers for j in (0, 1))
    named = first | second
    steps = jnp.arange(tok_rows)
    earlier = (steps[:, None] < steps[None, :]).astype(bf16)
    position = dot(named.astype(bf16), earlier, ((1,), (0,))).astype(jnp.int32)
    weight_of = jnp.where(first, route_weight[0][None], route_weight[1][None])
    chosen = named[:, None, :] & (
        position[:, None, :] == jnp.arange(capacity, dtype=jnp.int32)[None, :, None]
    )
    select = chosen.astype(bf16).reshape(experts_all * capacity, tok_rows)
    row_weight = jnp.sum(jnp.where(chosen, weight_of[:, None, :], 0.0), axis=2)
    both_in = jnp.concatenate([layer_in, out_cot], axis=1)
    scale = jnp.where(
        jnp.arange(2 * local_cols)[None] < local_cols, 1.0, row_weight.reshape(-1, 1)
    )
    send = (dot(select, both_in, ((1,), (0,))) * scale).astype(bf16)
    rows = experts_all * capacity
    own = lax.all_to_all(
        send.reshape(experts_all, capacity, 2 * local_cols), "sp", 0, 0, tiled=True
    ).reshape(rows, 2 * local_cols)
    other = swapped(own)
    x_pair = in_order(own[:, :local_cols], other[:, :local_cols])
    cot_pair = in_order(own[:, local_cols:], other[:, local_cols:])

    gate_mat, up_mat, down_mat = (gate_weight[0], up_weight[0], down_weight[0])
    gate_up = jnp.concatenate([gate_mat, up_mat])
    hidden_here = gate_mat.shape[0]
    wide = 2 * local_cols
    pieces = [(x_pair, cot_pair, chip)]
    x_now, cot_now = x_pair, cot_pair
    half = rows // 2
    for s in range(1, far):
        x_now, cot_now = onward(x_now, 1), onward(cot_now, 1)
        if s == 2:
            log_line = jnp.pad(total_log, (0, DV - DK))[None]
            leaving = jnp.pad(jnp.concatenate([state, log_line]), ((0, 7), (0, 0))).astype(bf16)
            leaving = jnp.broadcast_to(leaving[None], (experts_all, *leaving.shape))
            received = lax.all_to_all(after(leaving, pieces[-1][0]), "sp", 0, 0, tiled=True)
            span_states = received[:, :DK].astype(f32)
            span_logs = received[:, DK, :DK].astype(f32)
        pieces.append((x_now, cot_now, chip_at(-way * s)))
        pieces.append((swapped(x_now), swapped(cot_now), chip_at(way * s)))
    last = []
    for now in (x_now, cot_now):
        one = onward(jnp.where(core == 0, now[:half], now[half:]), 1)
        two = swapped(one)
        last.append(
            jnp.concatenate([jnp.where(core == 0, one, two), jnp.where(core == 0, two, one)])
        )
    pieces.append((*last, chip_at(far)))
    pre = jnp.zeros((rows, 2 * hidden_here), f32)
    hidden_cot = jnp.zeros((rows, hidden_here), f32)
    for x_piece, cot_piece, at in pieces:
        pre = pre + dot(x_piece, columns(gate_up, at, wide), ((1,), (1,)))
        hidden_cot = hidden_cot + dot(cot_piece, columns(down_mat, at, wide), ((1,), (1,)))
    gate_pre, up_pre = pre[:, :hidden_here], pre[:, hidden_here:]
    sigmoid_gate = jax.nn.sigmoid(gate_pre)
    active = gate_pre * sigmoid_gate
    hidden = (active * up_pre).astype(bf16)
    up_cot = (hidden_cot * active).astype(bf16)
    gate_cot = (
        hidden_cot * up_pre * sigmoid_gate * (1.0 + gate_pre * (1.0 - sigmoid_gate))
    ).astype(bf16)
    both_cot = jnp.concatenate([gate_cot, up_cot], axis=1)

    def back_columns(at, number, count):
        return jnp.concatenate(
            [columns(gate_up, 2 * at + (number ^ k), local_cols) for k in range(count)], axis=1
        )

    def other_part(s, behind):
        mat = back_columns(chip_at(-way * s), 1 - core, 1 if s == far else 2)
        cots = both_cot if behind is None else after(both_cot, behind)
        part = dot(cots, mat, ((1,), (0,))).astype(bf16)
        come = swapped(part)
        return part, (come[:half], come[half:])

    first, come = other_part(far, None)
    both_cot = after(both_cot, first)
    from_other = {far: come}
    halves = (both_cot[:half], both_cot[half:])
    moving = [None, None]
    sent = {}
    latest = None
    for s in range(far, -1, -1):
        mat = back_columns(chip_at(way * s), core, 1 if s == far else 2)
        for h in (0, 1):
            part = dot(halves[h], mat, ((1,), (0,)))
            if s:
                part = part + from_other[s][h].astype(f32)
            if s < far:
                come = after(moving[h], latest).astype(f32)
                part = part + jnp.pad(come, ((0, 0), (0, wide - come.shape[1])))
            if s:
                latest = part.astype(bf16)
            if s:
                sent[s, h] = latest
                moving[h] = onward(latest, 1)
            else:
                moving[h] = part[:, :local_cols] + swapped(part[:, local_cols:].astype(bf16))
        if s > 1:
            _, from_other[s - 1] = other_part(s - 1, sent[s, 0])
    back = jnp.concatenate([m.astype(bf16) for m in moving])
    returned = lax.all_to_all(
        back.reshape(experts_all, capacity, local_cols), "sp", 0, 0, tiled=True
    ).reshape(rows, local_cols)

    gate_up_g = jnp.zeros((2 * hidden_here, gate_mat.shape[1]), f32)
    down_g = jnp.zeros(down_mat.shape, f32)
    for k, (x_piece, cot_piece, at) in enumerate(pieces):
        cots = after((both_cot, hidden), sent[far - k // 2, 1])
        gate_up_g = lax.dynamic_update_slice_in_dim(
            gate_up_g, dot(cots[0], x_piece, ((0,), (0,))), at * wide, axis=1
        )
        down_g = lax.dynamic_update_slice_in_dim(
            down_g, dot(cots[1], cot_piece, ((0,), (0,))), at * wide, axis=1
        )
    gate_g, up_g = gate_up_g[:hidden_here], gate_up_g[hidden_here:]

    spans = jnp.arange(experts_all)
    between = (spans[None, :] > spans[:, None]) & (spans[None, :] < mine)
    weights = jnp.exp(jnp.dot(between.astype(f32), span_logs, precision=highest))
    weights = jnp.where((spans < mine)[:, None], weights, 0.0)
    entry_state = jnp.sum(weights[:, :, None] * span_states, axis=0)
    beyond = (spans[None, :] < spans[:, None]) & (spans[None, :] > mine)
    back_weights = jnp.exp(jnp.dot(beyond.astype(f32), span_logs, precision=highest))
    back_weights = jnp.where((spans > mine)[:, None], back_weights, 0.0)
    growth = jnp.exp(cumulative)
    shrink = jnp.exp(-cumulative)
    query_decayed = scaled_query * growth
    key_back = key_blk * shrink
    scores = jnp.where(causal, bmm("ncd,nsd->ncs", query_decayed, key_back), 0.0)
    block_state = jnp.stack(
        [jnp.exp(so)[:, None] * entry_state + st for so, st in before]
    )
    span_end = jnp.exp(total_log)[:, None] * entry_state + state
    outputs = bmm("ncs,nsv->ncv", scores, value_blk) + bmm(
        "ncd,ndv->ncv", query_decayed, block_state
    )
    mixer_out = outputs.reshape(tok_rows, DV).astype(bf16)

    routed_sum = dot(select, returned, ((0,), (0,)))
    mixed_own = (out_cot.astype(f32) + routed_sum).astype(bf16)
    mixed_pair = in_order(mixed_own, swapped(mixed_own))
    mixed = [(mixed_pair, chip)]
    for s in range(1, far):
        chunk = onward(mixed_pair, s)
        mixed.append((chunk, chip_at(-way * s)))
        mixed.append((swapped(chunk), chip_at(way * s)))
    chunk = onward(mixed_own, far)
    mixed.append((in_order(chunk, swapped(chunk)), chip_at(far)))
    full_cot = jnp.zeros((tok_rows, chips * wide), bf16)
    for chunk, at in mixed:
        full_cot = lax.dynamic_update_slice_in_dim(full_cot, chunk, at * wide, axis=1)
    mixer_cot = dot(full_cot, out_weight, ((1,), (0,)))
    proj = dot(full_cot, mixer_out, ((0,), (0,))).astype(bf16)
    proj = proj.reshape(experts_all, -1, DV)

    cot_blk = mixer_cot.reshape(blocks, BLOCK, DV)
    block_future = bmm("ncd,ncv->ndv", query_decayed, cot_blk)
    beyond_of, back_state, back_log = [None] * blocks, jnp.zeros((DK, DV), f32), jnp.zeros((DK,), f32)
    for n in range(blocks - 1, -1, -1):
        beyond_of[n] = (back_log, back_state)
        back_state = back_state * block_decay[n][:, None] + block_future[n]
        back_log = back_log + span_log[n, 0]
    leaving = jnp.broadcast_to(back_state.astype(bf16)[None], (experts_all, DK, DV))
    received = lax.all_to_all(
        jnp.concatenate([proj, leaving], axis=1), "sp", 0, 0, tiled=True
    )
    proj_grad = jnp.sum(received[:, :-DK].astype(f32), axis=0)
    back_states = received[:, -DK:].astype(f32)
    future_state = jnp.sum(back_weights[:, :, None] * back_states, axis=0)
    block_future_state = jnp.stack(
        [jnp.exp(lo)[:, None] * future_state + st for lo, st in beyond_of]
    )
    cot_values = jnp.where(causal, bmm("ncv,nsv->ncs", cot_blk, value_blk), 0.0)
    query_scaled_grad = growth * (
        bmm("ncv,ndv->ncd", cot_blk, block_state) + bmm("ncs,nsd->ncd", cot_values, key_back)
    )
    key_grad = shrink * bmm("ncs,ncd->nsd", cot_values, query_decayed) + to_end * bmm(
        "nsv,ndv->nsd", value_blk, block_future_state
    )
    value_grad = bmm("ncs,ncv->nsv", scores, cot_blk) + bmm(
        "nsd,ndv->nsv", key_to_end, block_future_state
    )
    terms = scaled_query * query_scaled_grad - key_blk * key_grad
    within_tail = jnp.einsum("cs,nsd->ncd", causal.T.astype(f32), terms, precision=highest)
    later_tail, tails = jnp.sum(future_state * span_end, axis=1), [None] * blocks
    for n in range(blocks - 1, -1, -1):
        tails[n] = within_tail[n] + later_tail[None]
        later_tail = later_tail + within_tail[n, 0]
    log_grad = jnp.stack(tails)
    logit_grad = log_grad * jax.nn.sigmoid(-logit_blk) / decay_temp
    flat = lambda a: a.reshape(tok_rows, -1)
    return (
        gate_g[None],
        up_g[None],
        down_g[None],
        proj_grad,
        flat(query_scaled_grad * DK ** (-0.5)),
        flat(key_grad),
        flat(value_grad),
        flat(logit_grad),
    )


def solution(mesh):
    in_specs = (
        P("sp", "tp"),
        P("sp", "tp"),
        P("sp", None),
        P("sp", None),
        P("sp"),
        P("sp", "tp", None),
        P("sp", "tp", None),
        P("sp", "tp", None),
        P(None, "tp"),
        P("sp", "tp"),
        P("sp", "tp"),
        P("sp", "tp"),
        P("sp", "tp"),
    )
    out_specs = (
        P("sp", "tp", None),
        P("sp", "tp", None),
        P("sp", "tp", None),
        P("sp", "tp"),
        P("sp", "tp"),
        P("sp", "tp"),
        P("sp", "tp"),
        P("sp", "tp"),
    )

    return jax.shard_map(local, mesh=mesh, in_specs=in_specs, out_specs=out_specs, check_vma=False)
```

```python
import jax
import jax.numpy as jnp
from jax import lax
from jax.sharding import PartitionSpec as P


DK = 64
DV = 128
BLOCK = 64


decay_temp = 16.0
highest = lax.Precision.HIGHEST
f32 = jnp.float32
bf16 = jnp.bfloat16


def dot(a, b, dims):
    return lax.dot_general(a, b, (dims, ((), ())), preferred_element_type=f32)


def onward(x, hops):
    size = lax.axis_size("tp")
    return lax.ppermute(
        x, "tp", [(i, (i + (2 * hops if i % 2 == 0 else -2 * hops)) % size) for i in range(size)]
    )


def swapped(x):
    return lax.ppermute(x, "tp", [(i, i ^ 1) for i in range(lax.axis_size("tp"))])


def columns(mat, block, width):
    return lax.dynamic_slice_in_dim(mat, block * width, width, axis=1)


def bmm(spec, a, b):
    return jnp.einsum(spec, a, b, precision=highest)


def local(
    layer_in,
    out_cot,
    route_ids,
    route_probs,
    group_prob,
    gate_weight,
    up_weight,
    down_weight,
    out_weight,
    query,
    key_in,
    value,
    decay_logit,
):
    tok_rows, local_cols = layer_in.shape
    experts_all = lax.axis_size("sp")
    capacity = 4 * tok_rows // experts_all
    chips = lax.axis_size("tp") // 2
    far = chips // 2
    place = lax.axis_index("tp")
    chip, core = place // 2, place % 2
    mine = lax.axis_index("sp")

    way = 1 - 2 * core

    def chip_at(distance):
        return (chip + distance) % chips

    def in_order(own, other):
        low = core == 0
        return jnp.concatenate([jnp.where(low, own, other), jnp.where(low, other, own)], axis=1)

    def after(x, y):
        return lax.optimization_barrier((x, y))[0]

    blocks = tok_rows // BLOCK
    split = lambda a: a.astype(f32).reshape(blocks, BLOCK, -1)
    scaled_query = split(query) * DK ** (-0.5)
    key_blk, value_blk, logit_blk = split(key_in), split(value), split(decay_logit)
    log_decay = jax.nn.log_sigmoid(logit_blk) / decay_temp
    causal = jnp.tril(jnp.ones((BLOCK, BLOCK), dtype=bool))
    cumulative = jnp.einsum(
        "cs,nsd->ncd", causal.astype(f32), log_decay, precision=highest
    )
    span_log = cumulative[:, -1:, :]
    to_end = jnp.exp(span_log - cumulative)
    key_to_end = key_blk * to_end
    block_decay = jnp.exp(span_log[:, 0, :])
    block_update = bmm("ncd,ncv->ndv", key_to_end, value_blk)
    before, state, so_far = [], jnp.zeros((DK, DV), f32), jnp.zeros((DK,), f32)
    for n in range(blocks):
        before.append((so_far, state))
        state = state * block_decay[n][:, None] + block_update[n]
        so_far = so_far + span_log[n, 0]
    total_log = so_far

    ids = route_ids.T
    probs = route_probs.T
    route_weight = group_prob[None] * probs / jnp.sum(probs, axis=0, keepdims=True)
    numbers = jnp.arange(experts_all, dtype=jnp.int32)[:, None]
    first, second = (ids[j][None] == numbers for j in (0, 1))
    named = first | second
    steps = jnp.arange(tok_rows)
    earlier = (steps[:, None] < steps[None, :]).astype(bf16)
    position = dot(named.astype(bf16), earlier, ((1,), (0,))).astype(jnp.int32)
    weight_of = jnp.where(first, route_weight[0][None], route_weight[1][None])
    chosen = named[:, None, :] & (
        position[:, None, :] == jnp.arange(capacity, dtype=jnp.int32)[None, :, None]
    )
    select = chosen.astype(bf16).reshape(experts_all * capacity, tok_rows)
    row_weight = jnp.sum(jnp.where(chosen, weight_of[:, None, :], 0.0), axis=2)
    both_in = jnp.concatenate([layer_in, out_cot], axis=1)
    scale = jnp.where(
        jnp.arange(2 * local_cols)[None] < local_cols, 1.0, row_weight.reshape(-1, 1)
    )
    send = (dot(select, both_in, ((1,), (0,))) * scale).astype(bf16)
    rows = experts_all * capacity
    own = lax.all_to_all(
        send.reshape(experts_all, capacity, 2 * local_cols), "sp", 0, 0, tiled=True
    ).reshape(rows, 2 * local_cols)
    other = swapped(own)
    x_pair = in_order(own[:, :local_cols], other[:, :local_cols])
    cot_pair = in_order(own[:, local_cols:], other[:, local_cols:])

    gate_mat, up_mat, down_mat = (gate_weight[0], up_weight[0], down_weight[0])
    gate_up = jnp.concatenate([gate_mat, up_mat])
    hidden_here = gate_mat.shape[0]
    wide = 2 * local_cols
    pieces = [(x_pair, cot_pair, chip)]
    x_now, cot_now = x_pair, cot_pair
    half = rows // 2
    for s in range(1, far):
        x_now, cot_now = onward(x_now, 1), onward(cot_now, 1)
        pieces.append((x_now, cot_now, chip_at(-way * s)))
        pieces.append((swapped(x_now), swapped(cot_now), chip_at(way * s)))
    last = []
    for now in (x_now, cot_now):
        one = onward(jnp.where(core == 0, now[:half], now[half:]), 1)
        two = swapped(one)
        last.append(
            jnp.concatenate([jnp.where(core == 0, one, two), jnp.where(core == 0, two, one)])
        )
    pieces.append((*last, chip_at(far)))
    pre = jnp.zeros((rows, 2 * hidden_here), f32)
    hidden_cot = jnp.zeros((rows, hidden_here), f32)
    for x_piece, cot_piece, at in pieces:
        pre = pre + dot(x_piece, columns(gate_up, at, wide), ((1,), (1,)))
        hidden_cot = hidden_cot + dot(cot_piece, columns(down_mat, at, wide), ((1,), (1,)))
    gate_pre, up_pre = pre[:, :hidden_here], pre[:, hidden_here:]
    sigmoid_gate = jax.nn.sigmoid(gate_pre)
    active = gate_pre * sigmoid_gate
    hidden = (active * up_pre).astype(bf16)
    up_cot = (hidden_cot * active).astype(bf16)
    gate_cot = (
        hidden_cot * up_pre * sigmoid_gate * (1.0 + gate_pre * (1.0 - sigmoid_gate))
    ).astype(bf16)
    both_cot = jnp.concatenate([gate_cot, up_cot], axis=1)

    def back_columns(at, number, count):
        return jnp.concatenate(
            [columns(gate_up, 2 * at + (number ^ k), local_cols) for k in range(count)], axis=1
        )

    def other_part(s, behind):
        mat = back_columns(chip_at(-way * s), 1 - core, 1 if s == far else 2)
        cots = both_cot if behind is None else after(both_cot, behind)
        part = dot(cots, mat, ((1,), (0,))).astype(bf16)
        come = swapped(part)
        return part, (come[:half], come[half:])

    first, come = other_part(far, None)
    both_cot = after(both_cot, first)
    from_other = {far: come}
    halves = (both_cot[:half], both_cot[half:])
    moving = [None, None]
    sent = {}
    latest = None
    for s in range(far, -1, -1):
        mat = back_columns(chip_at(way * s), core, 1 if s == far else 2)
        for h in (0, 1):
            part = dot(halves[h], mat, ((1,), (0,)))
            if s:
                part = part + from_other[s][h].astype(f32)
            if s < far:
                come = after(moving[h], latest).astype(f32)
                part = part + jnp.pad(come, ((0, 0), (0, wide - come.shape[1])))
            if s:
                latest = part.astype(bf16)
            if s:
                sent[s, h] = latest
                moving[h] = onward(latest, 1)
            else:
                moving[h] = part[:, :local_cols] + swapped(part[:, local_cols:].astype(bf16))
        if s > 1:
            _, from_other[s - 1] = other_part(s - 1, sent[s, 0])
    back = jnp.concatenate([m.astype(bf16) for m in moving])
    returned = lax.all_to_all(
        back.reshape(experts_all, capacity, local_cols), "sp", 0, 0, tiled=True
    ).reshape(rows, local_cols)

    gate_up_g = jnp.zeros((2 * hidden_here, gate_mat.shape[1]), f32)
    down_g = jnp.zeros(down_mat.shape, f32)
    for k, (x_piece, cot_piece, at) in enumerate(pieces):
        cots = after((both_cot, hidden), sent[far - k // 2, 1])
        gate_up_g = lax.dynamic_update_slice_in_dim(
            gate_up_g, dot(cots[0], x_piece, ((0,), (0,))), at * wide, axis=1
        )
        down_g = lax.dynamic_update_slice_in_dim(
            down_g, dot(cots[1], cot_piece, ((0,), (0,))), at * wide, axis=1
        )
    gate_g, up_g = gate_up_g[:hidden_here], gate_up_g[hidden_here:]

    routed_sum = dot(select, returned, ((0,), (0,)))
    mixed_own = (out_cot.astype(f32) + routed_sum).astype(bf16)
    mixed_pair = in_order(mixed_own, swapped(mixed_own))
    near = [onward(mixed_pair, s) for s in range(1, far)]
    last = onward(mixed_own, far)
    log_line = jnp.pad(total_log, (0, DV - DK))[None]
    leaving = jnp.pad(jnp.concatenate([state, log_line]), ((0, 7), (0, 0))).astype(bf16)
    leaving = jnp.broadcast_to(leaving[None], (experts_all, *leaving.shape))
    received = lax.all_to_all(after(leaving, mixed_own), "sp", 0, 0, tiled=True)
    span_states = received[:, :DK].astype(f32)
    span_logs = received[:, DK, :DK].astype(f32)
    come = swapped(jnp.concatenate([*near, last], axis=1))
    mixed = [(mixed_pair, chip)]
    for s in range(1, far):
        mixed.append((near[s - 1], chip_at(-way * s)))
        mixed.append((come[:, (s - 1) * wide : s * wide], chip_at(way * s)))
    mixed.append((in_order(last, come[:, (far - 1) * wide :]), chip_at(far)))
    full_cot = jnp.zeros((tok_rows, chips * wide), bf16)
    for chunk, at in mixed:
        full_cot = lax.dynamic_update_slice_in_dim(full_cot, chunk, at * wide, axis=1)
    spans = jnp.arange(experts_all)
    between = (spans[None, :] > spans[:, None]) & (spans[None, :] < mine)
    weights = jnp.exp(jnp.dot(between.astype(f32), span_logs, precision=highest))
    weights = jnp.where((spans < mine)[:, None], weights, 0.0)
    entry_state = jnp.sum(weights[:, :, None] * span_states, axis=0)
    beyond = (spans[None, :] < spans[:, None]) & (spans[None, :] > mine)
    back_weights = jnp.exp(jnp.dot(beyond.astype(f32), span_logs, precision=highest))
    back_weights = jnp.where((spans > mine)[:, None], back_weights, 0.0)
    growth = jnp.exp(cumulative)
    shrink = jnp.exp(-cumulative)
    query_decayed = scaled_query * growth
    key_back = key_blk * shrink
    scores = jnp.where(causal, bmm("ncd,nsd->ncs", query_decayed, key_back), 0.0)
    block_state = jnp.stack(
        [jnp.exp(so)[:, None] * entry_state + st for so, st in before]
    )
    span_end = jnp.exp(total_log)[:, None] * entry_state + state
    outputs = bmm("ncs,nsv->ncv", scores, value_blk) + bmm(
        "ncd,ndv->ncv", query_decayed, block_state
    )
    mixer_out = outputs.reshape(tok_rows, DV).astype(bf16)

    mixer_cot = dot(full_cot, out_weight, ((1,), (0,)))
    proj = dot(full_cot, mixer_out, ((0,), (0,))).astype(bf16)
    proj = proj.reshape(experts_all, -1, DV)

    cot_blk = mixer_cot.reshape(blocks, BLOCK, DV)
    block_future = bmm("ncd,ncv->ndv", query_decayed, cot_blk)
    beyond_of, back_state, back_log = [None] * blocks, jnp.zeros((DK, DV), f32), jnp.zeros((DK,), f32)
    for n in range(blocks - 1, -1, -1):
        beyond_of[n] = (back_log, back_state)
        back_state = back_state * block_decay[n][:, None] + block_future[n]
        back_log = back_log + span_log[n, 0]
    leaving = jnp.broadcast_to(back_state.astype(bf16)[None], (experts_all, DK, DV))
    received = lax.all_to_all(
        jnp.concatenate([proj, leaving], axis=1), "sp", 0, 0, tiled=True
    )
    proj_grad = jnp.sum(received[:, :-DK].astype(f32), axis=0)
    back_states = received[:, -DK:].astype(f32)
    future_state = jnp.sum(back_weights[:, :, None] * back_states, axis=0)
    block_future_state = jnp.stack(
        [jnp.exp(lo)[:, None] * future_state + st for lo, st in beyond_of]
    )
    cot_values = jnp.where(causal, bmm("ncv,nsv->ncs", cot_blk, value_blk), 0.0)
    query_scaled_grad = growth * (
        bmm("ncv,ndv->ncd", cot_blk, block_state) + bmm("ncs,nsd->ncd", cot_values, key_back)
    )
    key_grad = shrink * bmm("ncs,ncd->nsd", cot_values, query_decayed) + to_end * bmm(
        "nsv,ndv->nsd", value_blk, block_future_state
    )
    value_grad = bmm("ncs,ncv->nsv", scores, cot_blk) + bmm(
        "nsd,ndv->nsv", key_to_end, block_future_state
    )
    terms = scaled_query * query_scaled_grad - key_blk * key_grad
    within_tail = jnp.einsum("cs,nsd->ncd", causal.T.astype(f32), terms, precision=highest)
    later_tail, tails = jnp.sum(future_state * span_end, axis=1), [None] * blocks
    for n in range(blocks - 1, -1, -1):
        tails[n] = within_tail[n] + later_tail[None]
        later_tail = later_tail + within_tail[n, 0]
    log_grad = jnp.stack(tails)
    logit_grad = log_grad * jax.nn.sigmoid(-logit_blk) / decay_temp
    flat = lambda a: a.reshape(tok_rows, -1)
    return (
        gate_g[None],
        up_g[None],
        down_g[None],
        proj_grad,
        flat(query_scaled_grad * DK ** (-0.5)),
        flat(key_grad),
        flat(value_grad),
        flat(logit_grad),
    )


def solution(mesh):
    in_specs = (
        P("sp", "tp"),
        P("sp", "tp"),
        P("sp", None),
        P("sp", None),
        P("sp"),
        P("sp", "tp", None),
        P("sp", "tp", None),
        P("sp", "tp", None),
        P(None, "tp"),
        P("sp", "tp"),
        P("sp", "tp"),
        P("sp", "tp"),
        P("sp", "tp"),
    )
    out_specs = (
        P("sp", "tp", None),
        P("sp", "tp", None),
        P("sp", "tp", None),
        P("sp", "tp"),
        P("sp", "tp"),
        P("sp", "tp"),
        P("sp", "tp"),
        P("sp", "tp"),
    )

    return jax.shard_map(local, mesh=mesh, in_specs=in_specs, out_specs=out_specs, check_vma=False)
```

```python
import jax
import jax.numpy as jnp
from jax import lax
from jax.sharding import PartitionSpec as P


DK = 64
DV = 128
BLOCK = 64


decay_temp = 16.0
highest = lax.Precision.HIGHEST
f32 = jnp.float32
bf16 = jnp.bfloat16


def dot(a, b, dims):
    return lax.dot_general(a, b, (dims, ((), ())), preferred_element_type=f32)


def onward(x, hops):
    size = lax.axis_size("tp")
    return lax.ppermute(
        x, "tp", [(i, (i + (2 * hops if i % 2 == 0 else -2 * hops)) % size) for i in range(size)]
    )


def swapped(x):
    return lax.ppermute(x, "tp", [(i, i ^ 1) for i in range(lax.axis_size("tp"))])


def columns(mat, block, width):
    return lax.dynamic_slice_in_dim(mat, block * width, width, axis=1)


def bmm(spec, a, b):
    return jnp.einsum(spec, a, b, precision=highest)


def local(
    layer_in,
    out_cot,
    route_ids,
    route_probs,
    group_prob,
    gate_weight,
    up_weight,
    down_weight,
    out_weight,
    query,
    key_in,
    value,
    decay_logit,
):
    tok_rows, local_cols = layer_in.shape
    experts_all = lax.axis_size("sp")
    capacity = 4 * tok_rows // experts_all
    chips = lax.axis_size("tp") // 2
    far = chips // 2
    place = lax.axis_index("tp")
    chip, core = place // 2, place % 2
    mine = lax.axis_index("sp")

    way = 1 - 2 * core

    def chip_at(distance):
        return (chip + distance) % chips

    def in_order(own, other):
        low = core == 0
        return jnp.concatenate([jnp.where(low, own, other), jnp.where(low, other, own)], axis=1)

    def after(x, y):
        return lax.optimization_barrier((x, y))[0]

    ids = route_ids.T
    probs = route_probs.T
    route_weight = group_prob[None] * probs / jnp.sum(probs, axis=0, keepdims=True)
    numbers = jnp.arange(experts_all, dtype=jnp.int32)[:, None]
    first, second = (ids[j][None] == numbers for j in (0, 1))
    named = first | second
    steps = jnp.arange(tok_rows)
    earlier = (steps[:, None] < steps[None, :]).astype(bf16)
    position = dot(named.astype(bf16), earlier, ((1,), (0,))).astype(jnp.int32)
    weight_of = jnp.where(first, route_weight[0][None], route_weight[1][None])
    chosen = named[:, None, :] & (
        position[:, None, :] == jnp.arange(capacity, dtype=jnp.int32)[None, :, None]
    )
    select = chosen.astype(bf16).reshape(experts_all * capacity, tok_rows)
    row_weight = jnp.sum(jnp.where(chosen, weight_of[:, None, :], 0.0), axis=2)
    both_in = jnp.concatenate([layer_in, out_cot], axis=1)
    scale = jnp.where(
        jnp.arange(2 * local_cols)[None] < local_cols, 1.0, row_weight.reshape(-1, 1)
    )
    send = (dot(select, both_in, ((1,), (0,))) * scale).astype(bf16)
    rows = experts_all * capacity
    own = lax.all_to_all(
        send.reshape(experts_all, capacity, 2 * local_cols), "sp", 0, 0, tiled=True
    ).reshape(rows, 2 * local_cols)
    other = swapped(own)
    x_pair = in_order(own[:, :local_cols], other[:, :local_cols])
    cot_pair = in_order(own[:, local_cols:], other[:, local_cols:])

    gate_mat, up_mat, down_mat = (gate_weight[0], up_weight[0], down_weight[0])
    gate_up = jnp.concatenate([gate_mat, up_mat])
    hidden_here = gate_mat.shape[0]
    wide = 2 * local_cols
    pieces = [(x_pair, cot_pair, chip)]
    x_now, cot_now = x_pair, cot_pair
    half = rows // 2
    for s in range(1, far):
        x_now, cot_now = onward(x_now, 1), onward(cot_now, 1)
        pieces.append((x_now, cot_now, chip_at(-way * s)))
        pieces.append((swapped(x_now), swapped(cot_now), chip_at(way * s)))
    last = []
    for now in (x_now, cot_now):
        one = onward(jnp.where(core == 0, now[:half], now[half:]), 1)
        two = swapped(one)
        last.append(
            jnp.concatenate([jnp.where(core == 0, one, two), jnp.where(core == 0, two, one)])
        )
    pieces.append((*last, chip_at(far)))
    pre = jnp.zeros((rows, 2 * hidden_here), f32)
    hidden_cot = jnp.zeros((rows, hidden_here), f32)
    for x_piece, cot_piece, at in pieces:
        pre = pre + dot(x_piece, columns(gate_up, at, wide), ((1,), (1,)))
        hidden_cot = hidden_cot + dot(cot_piece, columns(down_mat, at, wide), ((1,), (1,)))
    gate_pre, up_pre = pre[:, :hidden_here], pre[:, hidden_here:]
    sigmoid_gate = jax.nn.sigmoid(gate_pre)
    active = gate_pre * sigmoid_gate
    hidden = (active * up_pre).astype(bf16)
    up_cot = (hidden_cot * active).astype(bf16)
    gate_cot = (
        hidden_cot * up_pre * sigmoid_gate * (1.0 + gate_pre * (1.0 - sigmoid_gate))
    ).astype(bf16)
    both_cot = jnp.concatenate([gate_cot, up_cot], axis=1)

    query, key_in, value, decay_logit = after(
        (query, key_in, value, decay_logit), pieces[1][0]
    )
    blocks = tok_rows // BLOCK
    split = lambda a: a.astype(f32).reshape(blocks, BLOCK, -1)
    scaled_query = split(query) * DK ** (-0.5)
    key_blk, value_blk, logit_blk = split(key_in), split(value), split(decay_logit)
    log_decay = jax.nn.log_sigmoid(logit_blk) / decay_temp
    causal = jnp.tril(jnp.ones((BLOCK, BLOCK), dtype=bool))
    cumulative = jnp.einsum(
        "cs,nsd->ncd", causal.astype(f32), log_decay, precision=highest
    )
    span_log = cumulative[:, -1:, :]
    to_end = jnp.exp(span_log - cumulative)
    key_to_end = key_blk * to_end
    block_decay = jnp.exp(span_log[:, 0, :])
    block_update = bmm("ncd,ncv->ndv", key_to_end, value_blk)
    before, state, so_far = [], jnp.zeros((DK, DV), f32), jnp.zeros((DK,), f32)
    for n in range(blocks):
        before.append((so_far, state))
        state = state * block_decay[n][:, None] + block_update[n]
        so_far = so_far + span_log[n, 0]
    total_log = so_far

    def back_columns(at, number, count):
        return jnp.concatenate(
            [columns(gate_up, 2 * at + (number ^ k), local_cols) for k in range(count)], axis=1
        )

    def other_part(s, behind):
        mat = back_columns(chip_at(-way * s), 1 - core, 1 if s == far else 2)
        cots = both_cot if behind is None else after(both_cot, behind)
        part = dot(cots, mat, ((1,), (0,))).astype(bf16)
        come = swapped(part)
        return part, (come[:half], come[half:])

    first, come = other_part(far, None)
    both_cot = after(both_cot, first)
    from_other = {far: come}
    halves = (both_cot[:half], both_cot[half:])
    moving = [None, None]
    sent = {}
    latest = None
    for s in range(far, -1, -1):
        mat = back_columns(chip_at(way * s), core, 1 if s == far else 2)
        for h in (0, 1):
            part = dot(halves[h], mat, ((1,), (0,)))
            if s:
                part = part + from_other[s][h].astype(f32)
            if s < far:
                come = after(moving[h], latest).astype(f32)
                part = part + jnp.pad(come, ((0, 0), (0, wide - come.shape[1])))
            if s:
                latest = part.astype(bf16)
            if s:
                sent[s, h] = latest
                moving[h] = onward(latest, 1)
            else:
                moving[h] = part[:, :local_cols] + swapped(part[:, local_cols:].astype(bf16))
        if s > 1:
            _, from_other[s - 1] = other_part(s - 1, sent[s, 0])
    back = jnp.concatenate([m.astype(bf16) for m in moving])
    returned = lax.all_to_all(
        back.reshape(experts_all, capacity, local_cols), "sp", 0, 0, tiled=True
    ).reshape(rows, local_cols)

    routed_sum = dot(select, returned, ((0,), (0,)))
    mixed_own = (out_cot.astype(f32) + routed_sum).astype(bf16)
    mixed_pair = in_order(mixed_own, swapped(mixed_own))
    near = [onward(mixed_pair, s) for s in range(1, far)]
    last = onward(mixed_own, far)
    log_line = jnp.pad(total_log, (0, DV - DK))[None]
    leaving = jnp.pad(jnp.concatenate([state, log_line]), ((0, 7), (0, 0))).astype(bf16)
    leaving = jnp.broadcast_to(leaving[None], (experts_all, *leaving.shape))
    received = lax.all_to_all(after(leaving, mixed_own), "sp", 0, 0, tiled=True)
    span_states = received[:, :DK].astype(f32)
    span_logs = received[:, DK, :DK].astype(f32)
    come = swapped(jnp.concatenate([*near, last], axis=1))
    mixed = [(mixed_pair, chip)]
    for s in range(1, far):
        mixed.append((near[s - 1], chip_at(-way * s)))
        mixed.append((come[:, (s - 1) * wide : s * wide], chip_at(way * s)))
    mixed.append((in_order(last, come[:, (far - 1) * wide :]), chip_at(far)))
    full_cot = jnp.zeros((tok_rows, chips * wide), bf16)
    for chunk, at in mixed:
        full_cot = lax.dynamic_update_slice_in_dim(full_cot, chunk, at * wide, axis=1)
    spans = jnp.arange(experts_all)
    between = (spans[None, :] > spans[:, None]) & (spans[None, :] < mine)
    weights = jnp.exp(jnp.dot(between.astype(f32), span_logs, precision=highest))
    weights = jnp.where((spans < mine)[:, None], weights, 0.0)
    entry_state = jnp.sum(weights[:, :, None] * span_states, axis=0)
    beyond = (spans[None, :] < spans[:, None]) & (spans[None, :] > mine)
    back_weights = jnp.exp(jnp.dot(beyond.astype(f32), span_logs, precision=highest))
    back_weights = jnp.where((spans > mine)[:, None], back_weights, 0.0)
    growth = jnp.exp(cumulative)
    shrink = jnp.exp(-cumulative)
    query_decayed = scaled_query * growth
    key_back = key_blk * shrink
    scores = jnp.where(causal, bmm("ncd,nsd->ncs", query_decayed, key_back), 0.0)
    block_state = jnp.stack(
        [jnp.exp(so)[:, None] * entry_state + st for so, st in before]
    )
    span_end = jnp.exp(total_log)[:, None] * entry_state + state
    outputs = bmm("ncs,nsv->ncv", scores, value_blk) + bmm(
        "ncd,ndv->ncv", query_decayed, block_state
    )
    mixer_out = outputs.reshape(tok_rows, DV).astype(bf16)

    mixer_cot = dot(full_cot, out_weight, ((1,), (0,)))
    proj = dot(full_cot, mixer_out, ((0,), (0,))).astype(bf16)
    proj = proj.reshape(experts_all, -1, DV)

    cot_blk = mixer_cot.reshape(blocks, BLOCK, DV)
    block_future = bmm("ncd,ncv->ndv", query_decayed, cot_blk)
    beyond_of, back_state, back_log = [None] * blocks, jnp.zeros((DK, DV), f32), jnp.zeros((DK,), f32)
    for n in range(blocks - 1, -1, -1):
        beyond_of[n] = (back_log, back_state)
        back_state = back_state * block_decay[n][:, None] + block_future[n]
        back_log = back_log + span_log[n, 0]
    leaving = jnp.broadcast_to(back_state.astype(bf16)[None], (experts_all, DK, DV))
    leaving = jnp.concatenate([proj, leaving], axis=1)
    received = lax.all_to_all(leaving, "sp", 0, 0, tiled=True)
    proj_grad = jnp.sum(received[:, :-DK].astype(f32), axis=0)
    back_states = received[:, -DK:].astype(f32)
    future_state = jnp.sum(back_weights[:, :, None] * back_states, axis=0)
    block_future_state = jnp.stack(
        [jnp.exp(lo)[:, None] * future_state + st for lo, st in beyond_of]
    )
    cot_values = jnp.where(causal, bmm("ncv,nsv->ncs", cot_blk, value_blk), 0.0)
    query_scaled_grad = growth * (
        bmm("ncv,ndv->ncd", cot_blk, block_state) + bmm("ncs,nsd->ncd", cot_values, key_back)
    )
    key_grad = shrink * bmm("ncs,ncd->nsd", cot_values, query_decayed) + to_end * bmm(
        "nsv,ndv->nsd", value_blk, block_future_state
    )
    value_grad = bmm("ncs,ncv->nsv", scores, cot_blk) + bmm(
        "nsd,ndv->nsv", key_to_end, block_future_state
    )
    terms = scaled_query * query_scaled_grad - key_blk * key_grad
    within_tail = jnp.einsum("cs,nsd->ncd", causal.T.astype(f32), terms, precision=highest)
    later_tail, tails = jnp.sum(future_state * span_end, axis=1), [None] * blocks
    for n in range(blocks - 1, -1, -1):
        tails[n] = within_tail[n] + later_tail[None]
        later_tail = later_tail + within_tail[n, 0]
    log_grad = jnp.stack(tails)
    logit_grad = log_grad * jax.nn.sigmoid(-logit_blk) / decay_temp
    behind = [(sent[4, 1], sent[3, 0]), (sent[3, 1], sent[2, 0]), (sent[2, 1], sent[1, 0])]
    behind += [(back, back), (back, back), (mixed_own, mixed_own), (leaving, leaving)]
    behind += [(leaving, leaving)]
    gate_up_g = jnp.zeros((2 * hidden_here, gate_mat.shape[1]), f32)
    down_g = jnp.zeros(down_mat.shape, f32)
    for k, (x_piece, cot_piece, at) in enumerate(pieces):
        gate_up_g = lax.dynamic_update_slice_in_dim(
            gate_up_g,
            dot(after(both_cot, behind[k][0]), x_piece, ((0,), (0,))),
            at * wide,
            axis=1,
        )
        down_g = lax.dynamic_update_slice_in_dim(
            down_g,
            dot(after(hidden, behind[k][1]), cot_piece, ((0,), (0,))),
            at * wide,
            axis=1,
        )
    gate_g, up_g = gate_up_g[:hidden_here], gate_up_g[hidden_here:]
    flat = lambda a: a.reshape(tok_rows, -1)
    return (
        gate_g[None],
        up_g[None],
        down_g[None],
        proj_grad,
        flat(query_scaled_grad * DK ** (-0.5)),
        flat(key_grad),
        flat(value_grad),
        flat(logit_grad),
    )


def solution(mesh):
    in_specs = (
        P("sp", "tp"),
        P("sp", "tp"),
        P("sp", None),
        P("sp", None),
        P("sp"),
        P("sp", "tp", None),
        P("sp", "tp", None),
        P("sp", "tp", None),
        P(None, "tp"),
        P("sp", "tp"),
        P("sp", "tp"),
        P("sp", "tp"),
        P("sp", "tp"),
    )
    out_specs = (
        P("sp", "tp", None),
        P("sp", "tp", None),
        P("sp", "tp", None),
        P("sp", "tp"),
        P("sp", "tp"),
        P("sp", "tp"),
        P("sp", "tp"),
        P("sp", "tp"),
    )

    return jax.shard_map(local, mesh=mesh, in_specs=in_specs, out_specs=out_specs, check_vma=False)
```

```python
import jax
import jax.numpy as jnp
from jax import lax
from jax.sharding import PartitionSpec as P


DK = 64
DV = 128
BLOCK = 64


decay_temp = 16.0
highest = lax.Precision.HIGHEST
f32 = jnp.float32
bf16 = jnp.bfloat16


def dot(a, b, dims):
    return lax.dot_general(a, b, (dims, ((), ())), preferred_element_type=f32)


def onward(x, hops):
    size = lax.axis_size("tp")
    return lax.ppermute(
        x, "tp", [(i, (i + (2 * hops if i % 2 == 0 else -2 * hops)) % size) for i in range(size)]
    )


def swapped(x):
    return lax.ppermute(x, "tp", [(i, i ^ 1) for i in range(lax.axis_size("tp"))])


def columns(mat, block, width):
    return lax.dynamic_slice_in_dim(mat, block * width, width, axis=1)


def bmm(spec, a, b):
    return jnp.einsum(spec, a, b, precision=highest)


def local(
    layer_in,
    out_cot,
    route_ids,
    route_probs,
    group_prob,
    gate_weight,
    up_weight,
    down_weight,
    out_weight,
    query,
    key_in,
    value,
    decay_logit,
):
    tok_rows, local_cols = layer_in.shape
    experts_all = lax.axis_size("sp")
    capacity = 4 * tok_rows // experts_all
    chips = lax.axis_size("tp") // 2
    far = chips // 2
    place = lax.axis_index("tp")
    chip, core = place // 2, place % 2
    mine = lax.axis_index("sp")

    way = 1 - 2 * core

    def chip_at(distance):
        return (chip + distance) % chips

    def in_order(own, other):
        low = core == 0
        return jnp.concatenate([jnp.where(low, own, other), jnp.where(low, other, own)], axis=1)

    def after(x, y):
        return lax.optimization_barrier((x, y))[0]

    ids = route_ids.T
    probs = route_probs.T
    route_weight = group_prob[None] * probs / jnp.sum(probs, axis=0, keepdims=True)
    numbers = jnp.arange(experts_all, dtype=jnp.int32)[:, None]
    first, second = (ids[j][None] == numbers for j in (0, 1))
    named = first | second
    steps = jnp.arange(tok_rows)
    earlier = (steps[:, None] < steps[None, :]).astype(bf16)
    position = dot(named.astype(bf16), earlier, ((1,), (0,))).astype(jnp.int32)
    weight_of = jnp.where(first, route_weight[0][None], route_weight[1][None])
    chosen = named[:, None, :] & (
        position[:, None, :] == jnp.arange(capacity, dtype=jnp.int32)[None, :, None]
    )
    select = chosen.astype(bf16).reshape(experts_all * capacity, tok_rows)
    row_weight = jnp.sum(jnp.where(chosen, weight_of[:, None, :], 0.0), axis=2)
    both_in = jnp.concatenate([layer_in, out_cot], axis=1)
    scale = jnp.where(
        jnp.arange(2 * local_cols)[None] < local_cols, 1.0, row_weight.reshape(-1, 1)
    )
    send = (dot(select, both_in, ((1,), (0,))) * scale).astype(bf16)
    rows = experts_all * capacity
    own = lax.all_to_all(
        send.reshape(experts_all, capacity, 2 * local_cols), "sp", 0, 0, tiled=True
    ).reshape(rows, 2 * local_cols)
    other = swapped(own)
    x_pair = in_order(own[:, :local_cols], other[:, :local_cols])
    cot_pair = in_order(own[:, local_cols:], other[:, local_cols:])

    gate_mat, up_mat, down_mat = (gate_weight[0], up_weight[0], down_weight[0])
    gate_up = jnp.concatenate([gate_mat, up_mat])
    hidden_here = gate_mat.shape[0]
    wide = 2 * local_cols
    pieces = [(x_pair, cot_pair, chip)]
    x_now, cot_now = x_pair, cot_pair
    half = rows // 2
    for s in range(1, far):
        x_now, cot_now = onward(x_now, 1), onward(cot_now, 1)
        pieces.append((x_now, cot_now, chip_at(-way * s)))
        pieces.append((swapped(x_now), swapped(cot_now), chip_at(way * s)))
    last = []
    for now in (x_now, cot_now):
        one = onward(jnp.where(core == 0, now[:half], now[half:]), 1)
        two = swapped(one)
        last.append(
            jnp.concatenate([jnp.where(core == 0, one, two), jnp.where(core == 0, two, one)])
        )
    pieces.append((*last, chip_at(far)))
    pre = jnp.zeros((rows, 2 * hidden_here), f32)
    hidden_cot = jnp.zeros((rows, hidden_here), f32)
    for x_piece, cot_piece, at in pieces:
        pre = pre + dot(x_piece, columns(gate_up, at, wide), ((1,), (1,)))
        hidden_cot = hidden_cot + dot(cot_piece, columns(down_mat, at, wide), ((1,), (1,)))
    gate_pre, up_pre = pre[:, :hidden_here], pre[:, hidden_here:]
    sigmoid_gate = jax.nn.sigmoid(gate_pre)
    active = gate_pre * sigmoid_gate
    hidden = (active * up_pre).astype(bf16)
    up_cot = (hidden_cot * active).astype(bf16)
    gate_cot = (
        hidden_cot * up_pre * sigmoid_gate * (1.0 + gate_pre * (1.0 - sigmoid_gate))
    ).astype(bf16)
    both_cot = jnp.concatenate([gate_cot, up_cot], axis=1)

    query, key_in, value, decay_logit = after(
        (query, key_in, value, decay_logit), pieces[1][0]
    )
    blocks = tok_rows // BLOCK
    split = lambda a: a.astype(f32).reshape(blocks, BLOCK, -1)
    scaled_query = split(query) * DK ** (-0.5)
    key_blk, value_blk, logit_blk = split(key_in), split(value), split(decay_logit)
    log_decay = jax.nn.log_sigmoid(logit_blk) / decay_temp
    causal = jnp.tril(jnp.ones((BLOCK, BLOCK), dtype=bool))
    cumulative = jnp.einsum(
        "cs,nsd->ncd", causal.astype(f32), log_decay, precision=highest
    )
    span_log = cumulative[:, -1:, :]
    to_end = jnp.exp(span_log - cumulative)
    key_to_end = key_blk * to_end
    block_decay = jnp.exp(span_log[:, 0, :])
    block_update = bmm("ncd,ncv->ndv", key_to_end, value_blk)
    before, state, so_far = [], jnp.zeros((DK, DV), f32), jnp.zeros((DK,), f32)
    for n in range(blocks):
        before.append((so_far, state))
        state = state * block_decay[n][:, None] + block_update[n]
        so_far = so_far + span_log[n, 0]
    total_log = so_far

    def back_columns(at, number, count):
        return jnp.concatenate(
            [columns(gate_up, 2 * at + (number ^ k), local_cols) for k in range(count)], axis=1
        )

    def other_part(s, behind):
        mat = back_columns(chip_at(-way * s), 1 - core, 1 if s == far else 2)
        cots = both_cot if behind is None else after(both_cot, behind)
        part = dot(cots, mat, ((1,), (0,))).astype(bf16)
        come = swapped(part)
        return part, (come[:half], come[half:])

    first, come = other_part(far, None)
    both_cot = after(both_cot, first)
    from_other = {far: come}
    halves = (both_cot[:half], both_cot[half:])
    moving = [None, None]
    sent = {}
    latest = None
    for s in range(far, -1, -1):
        mat = back_columns(chip_at(way * s), core, 1 if s == far else 2)
        for h in (0, 1):
            part = dot(halves[h], mat, ((1,), (0,)))
            if s:
                part = part + from_other[s][h].astype(f32)
            if s < far:
                come = after(moving[h], latest).astype(f32)
                part = part + jnp.pad(come, ((0, 0), (0, wide - come.shape[1])))
            if s:
                latest = part.astype(bf16)
            if s:
                sent[s, h] = latest
                moving[h] = onward(latest, 1)
            else:
                moving[h] = part[:, :local_cols] + swapped(part[:, local_cols:].astype(bf16))
        if s > 1:
            _, from_other[s - 1] = other_part(s - 1, sent[s, 0])
    back = jnp.concatenate([m.astype(bf16) for m in moving])
    behind = [sent[at] for at in ((4, 1), (4, 1), (4, 1), (3, 1), (2, 1), (1, 1), (1, 1), (1, 1))]
    gate_up_g = jnp.zeros((2 * hidden_here, gate_mat.shape[1]), f32)
    down_g = jnp.zeros(down_mat.shape, f32)
    for k, (x_piece, cot_piece, at) in enumerate(pieces):
        gate_up_g = lax.dynamic_update_slice_in_dim(
            gate_up_g,
            dot(after(both_cot, behind[k]), x_piece, ((0,), (0,))),
            at * wide,
            axis=1,
        )
        down_g = lax.dynamic_update_slice_in_dim(
            down_g,
            dot(after(hidden, behind[k]), cot_piece, ((0,), (0,))),
            at * wide,
            axis=1,
        )
    gate_g, up_g = gate_up_g[:hidden_here], gate_up_g[hidden_here:]
    back = after(back, (gate_up_g, down_g))

    log_line = jnp.pad(total_log, (0, DV - DK))[None]
    leaving = jnp.pad(jnp.concatenate([state, log_line]), ((0, 7), (0, 0))).astype(bf16)
    leaving = jnp.broadcast_to(leaving[None], (experts_all, *leaving.shape))
    leaving = jnp.concatenate([back.reshape(experts_all, capacity, local_cols), leaving], axis=1)
    received = lax.all_to_all(leaving, "sp", 0, 0, tiled=True)
    returned = received[:, :capacity].reshape(rows, local_cols)
    span_states = received[:, capacity : capacity + DK].astype(f32)
    span_logs = received[:, capacity + DK, :DK].astype(f32)

    routed_sum = dot(select, returned, ((0,), (0,)))
    mixed_own = (out_cot.astype(f32) + routed_sum).astype(bf16)
    mixed_pair = in_order(mixed_own, swapped(mixed_own))
    near = [onward(mixed_pair, s) for s in range(1, far)]
    last = onward(mixed_own, far)
    come = swapped(jnp.concatenate([*near, last], axis=1))
    mixed = [(mixed_pair, chip)]
    for s in range(1, far):
        mixed.append((near[s - 1], chip_at(-way * s)))
        mixed.append((come[:, (s - 1) * wide : s * wide], chip_at(way * s)))
    mixed.append((in_order(last, come[:, (far - 1) * wide :]), chip_at(far)))
    full_cot = jnp.zeros((tok_rows, chips * wide), bf16)
    for chunk, at in mixed:
        full_cot = lax.dynamic_update_slice_in_dim(full_cot, chunk, at * wide, axis=1)
    spans = jnp.arange(experts_all)
    between = (spans[None, :] > spans[:, None]) & (spans[None, :] < mine)
    weights = jnp.exp(jnp.dot(between.astype(f32), span_logs, precision=highest))
    weights = jnp.where((spans < mine)[:, None], weights, 0.0)
    entry_state = jnp.sum(weights[:, :, None] * span_states, axis=0)
    beyond = (spans[None, :] < spans[:, None]) & (spans[None, :] > mine)
    back_weights = jnp.exp(jnp.dot(beyond.astype(f32), span_logs, precision=highest))
    back_weights = jnp.where((spans > mine)[:, None], back_weights, 0.0)
    growth = jnp.exp(cumulative)
    shrink = jnp.exp(-cumulative)
    query_decayed = scaled_query * growth
    key_back = key_blk * shrink
    scores = jnp.where(causal, bmm("ncd,nsd->ncs", query_decayed, key_back), 0.0)
    block_state = jnp.stack(
        [jnp.exp(so)[:, None] * entry_state + st for so, st in before]
    )
    span_end = jnp.exp(total_log)[:, None] * entry_state + state
    outputs = bmm("ncs,nsv->ncv", scores, value_blk) + bmm(
        "ncd,ndv->ncv", query_decayed, block_state
    )
    mixer_out = outputs.reshape(tok_rows, DV).astype(bf16)

    mixer_cot = dot(full_cot, out_weight, ((1,), (0,)))
    proj = dot(full_cot, mixer_out, ((0,), (0,))).astype(bf16)
    proj = proj.reshape(experts_all, -1, DV)

    cot_blk = mixer_cot.reshape(blocks, BLOCK, DV)
    block_future = bmm("ncd,ncv->ndv", query_decayed, cot_blk)
    beyond_of, back_state, back_log = [None] * blocks, jnp.zeros((DK, DV), f32), jnp.zeros((DK,), f32)
    for n in range(blocks - 1, -1, -1):
        beyond_of[n] = (back_log, back_state)
        back_state = back_state * block_decay[n][:, None] + block_future[n]
        back_log = back_log + span_log[n, 0]
    leaving = jnp.broadcast_to(back_state.astype(bf16)[None], (experts_all, DK, DV))
    leaving = jnp.concatenate([proj, leaving], axis=1)
    received = lax.all_to_all(leaving, "sp", 0, 0, tiled=True)
    proj_grad = jnp.sum(received[:, :-DK].astype(f32), axis=0)
    back_states = received[:, -DK:].astype(f32)
    future_state = jnp.sum(back_weights[:, :, None] * back_states, axis=0)
    block_future_state = jnp.stack(
        [jnp.exp(lo)[:, None] * future_state + st for lo, st in beyond_of]
    )
    cot_values = jnp.where(causal, bmm("ncv,nsv->ncs", cot_blk, value_blk), 0.0)
    query_scaled_grad = growth * (
        bmm("ncv,ndv->ncd", cot_blk, block_state) + bmm("ncs,nsd->ncd", cot_values, key_back)
    )
    key_grad = shrink * bmm("ncs,ncd->nsd", cot_values, query_decayed) + to_end * bmm(
        "nsv,ndv->nsd", value_blk, block_future_state
    )
    value_grad = bmm("ncs,ncv->nsv", scores, cot_blk) + bmm(
        "nsd,ndv->nsv", key_to_end, block_future_state
    )
    terms = scaled_query * query_scaled_grad - key_blk * key_grad
    within_tail = jnp.einsum("cs,nsd->ncd", causal.T.astype(f32), terms, precision=highest)
    later_tail, tails = jnp.sum(future_state * span_end, axis=1), [None] * blocks
    for n in range(blocks - 1, -1, -1):
        tails[n] = within_tail[n] + later_tail[None]
        later_tail = later_tail + within_tail[n, 0]
    log_grad = jnp.stack(tails)
    logit_grad = log_grad * jax.nn.sigmoid(-logit_blk) / decay_temp
    flat = lambda a: a.reshape(tok_rows, -1)
    return (
        gate_g[None],
        up_g[None],
        down_g[None],
        proj_grad,
        flat(query_scaled_grad * DK ** (-0.5)),
        flat(key_grad),
        flat(value_grad),
        flat(logit_grad),
    )


def solution(mesh):
    in_specs = (
        P("sp", "tp"),
        P("sp", "tp"),
        P("sp", None),
        P("sp", None),
        P("sp"),
        P("sp", "tp", None),
        P("sp", "tp", None),
        P("sp", "tp", None),
        P(None, "tp"),
        P("sp", "tp"),
        P("sp", "tp"),
        P("sp", "tp"),
        P("sp", "tp"),
    )
    out_specs = (
        P("sp", "tp", None),
        P("sp", "tp", None),
        P("sp", "tp", None),
        P("sp", "tp"),
        P("sp", "tp"),
        P("sp", "tp"),
        P("sp", "tp"),
        P("sp", "tp"),
    )

    return jax.shard_map(local, mesh=mesh, in_specs=in_specs, out_specs=out_specs, check_vma=False)
```
